32 devices in a mesh: ep: 4 (over y, x), tp: 8 (over z, core).
Axes of the slice: x: 2, y: 2, z: 4, core: 2. Of those that a mesh axis runs over, the one named last changes fastest.
Arguments:
- hidden_in: bfloat16 [64, 4096], P('ep'), may hold values from -6 to 6
- attn_gain: float32 [4096], replicated, may hold values from 0.1 to 1.9
- query_weight: bfloat16 [4096, 4096], P('ep', 'tp'), may hold values from -0.09375 to 0.09375
- key_weight: bfloat16 [4096, 1024], P('ep', 'tp'), may hold values from -0.09375 to 0.09375
- value_weight: bfloat16 [4096, 1024], P('ep', 'tp'), may hold values from -0.09375 to 0.09375
- query_gain: float32 [128], replicated, may hold values from 0.1 to 1.9
- key_gain: float32 [128], replicated, may hold values from 0.1 to 1.9
- head_offset: float32 [32], P('tp'), may hold values from -7 to -2
- key_cache: bfloat16 [64, 1024, 1024], P('ep', None, 'tp'), may hold values from -6 to 6
- value_cache: bfloat16 [64, 1024, 1024], P('ep', None, 'tp'), may hold values from -6 to 6
- lengths: int32 [64], P('ep'), may hold values from 1 to 1024
- out_weight: bfloat16 [4096, 4096], P('tp', 'ep'), may hold values from -0.375 to 0.375
- expert_gain: float32 [4096], replicated, may hold values from 0.1 to 1.9
- routes: int32 [64, 2], P('ep'), may hold values from 0 to 3, all different within a row; in each aligned block of 16 rows (0 to 15, 16 to 31, ...) at most 16 rows name the same one
- route_weights: float32 [64, 2], P('ep'), may hold values from 0.1 to 1
- gate_weight: bfloat16 [4, 4096, 2048], P('ep', None, 'tp'), may hold values from -0.09375 to 0.09375
- up_weight: bfloat16 [4, 4096, 2048], P('ep', None, 'tp'), may hold values from -0.09375 to 0.09375
- down_weight: bfloat16 [4, 2048, 4096], P('ep', 'tp'), may hold values from -0.125 to 0.125
Outputs:
- layer_out: bfloat16 [64, 4096], P('ep', 'tp')
- fresh_keys: bfloat16 [64, 1024], P('ep', 'tp')
- fresh_values: bfloat16 [64, 1024], P('ep', 'tp')
The draws below stay inside these ranges and needn't reach their ends.
Inputs may be any that keep to these rules, and one draw needn't show every extreme that they name: `routes`: each row names 2 different experts. Among the rows of one index of ep (16 rows) no expert is named more than 16 times, a bound that some block reaches.
All inputs are finite; a program needn't handle non-finite values.
Results may differ from the reference program's by a relative error of at most 0.018.
Values may be sent and summed in bfloat16 or wider, within the bound.
A program may use at most 64 MiB of HBM per device.

```python
import math
import jax
import jax.numpy as jnp
import numpy as np
from jax import lax

D = 4096
HEADS = 32
HD = 128
D_EXP = 2048
TOPK = 2
SEQ_DEV = 16
CACHE = 1024
KV_HEADS = 8
EXPERTS = 4
SEQS = 64
CAP = 16


def set_ends(entries, rng, least, top_value):
    shape = entries.shape
    place = [jax.random.randint(jax.random.fold_in(rng, axis), (), 0, shape[axis]) for axis in range(len(shape))]
    entries = entries.at[tuple(place)].set(least)
    longest = shape.index(max(shape))
    place[longest] = (place[longest] + 1) % shape[longest]
    return entries.at[tuple(place)].set(top_value)


def level_of(stream_key, extent, split, smallest, largest):
    level = 1.0
    for axis_at, shards_of in split:
        heights = jax.random.uniform(jax.random.fold_in(jax.random.fold_in(stream_key, 6), axis_at), (shards_of,), jnp.float32, smallest / len(split), largest / len(split))
        level = level * jnp.repeat(jnp.exp(heights), extent[axis_at] // shards_of).reshape((-1,) + (1,) * (len(extent) - 1 - axis_at))
    return level


def routed_block(key, own, number, rows, count, top, most, lean):
    order = jax.random.permutation(key, count)
    crowded, usual = portions_of(count, rows * top, most, lean, True), portions_of(count, rows * top, most, lean, False)
    places = jnp.arange(count)

    def named(tallies, rotation):
        used = int((tallies > 0).sum())
        fixed = max(1, used // 4)
        passed = fixed + (places - fixed + rotation * (used - fixed)) % max(1, count - fixed)
        return jnp.zeros((count,), jnp.int32).at[order[jnp.where(places < fixed, places, passed)]].set(jnp.asarray(tallies, jnp.int32))

    tallies = jnp.where(number % 4 == 0, named(crowded, number // 4), named(usual, number - number // 4 - 1))
    mixed = jax.random.permutation(jax.random.fold_in(own, 3), count)
    giver, taker = mixed[0:count // 2 * 2:2], mixed[1:count // 2 * 2:2]
    room = jnp.minimum(tallies[giver] - 1, most - tallies[taker]) // 2
    room = jnp.where((giver == order[0]) | (taker == order[0]) | (tallies[taker] == 0), 0, jnp.maximum(room, 0))
    passed = jax.random.randint(jax.random.fold_in(own, 4), (count // 2,), 0, 1 << 20) % (room + 1)
    tallies = tallies.at[giver].add(-passed).at[taker].add(passed)
    labels = jnp.searchsorted(jnp.cumsum(tallies), jnp.arange(rows * top), side="right").astype(jnp.int32)
    grid = labels.reshape(top, rows).T
    grid = grid[jax.random.permutation(jax.random.fold_in(own, 1), rows)]
    rotation = jax.random.randint(jax.random.fold_in(own, 2), (rows, 1), 0, top)
    return jnp.take_along_axis(grid, (jnp.arange(top)[None, :] + rotation) % top, axis=1)


def portions_of(number_of, total, limit, lean, full):
    loads = [(1 << 20) // math.isqrt(rank ** lean) + 1 for rank in range(1, number_of + 1)]
    largest = limit if full else min(limit, max(-(-total // number_of), total * loads[0] // sum(loads)))
    least = 1 if total - largest >= number_of - 1 else 0
    given, rest = [largest] + [least] * (number_of - 1), total - largest - least * (number_of - 1)
    while rest > 0:
        candidates = [i for i in range(1, number_of) if given[i] < largest] or [i for i in range(1, number_of) if given[i] < limit]
        whole, remaining = sum([loads[i] for i in candidates]), rest
        for i in candidates:
            more = min(limit - given[i], max(1, remaining * loads[i] // whole), rest)
            given[i] = given[i] + more
            rest = rest - more
    return np.array(given)


def gaussian(stream_key, shape, spread, limit, pieces=(), kind=jnp.bfloat16):
    entries = jax.random.normal(stream_key, shape, jnp.float32) * spread
    if len(pieces) > 0:
        entries = level_of(stream_key, shape, pieces, -0.22, 0.18) * entries
    return jnp.clip(entries, min=-limit, max=limit).astype(kind)


def setup_inputs(seed: int = 0) -> dict:
    arg_keys = jax.random.split(jax.random.key(seed), 19)
    hidden_in = gaussian(arg_keys[0], (SEQS, D), 1.0, 6.0, ((0, 4),))
    attn_gain = jnp.clip(1.0 + 0.18 * jax.random.normal(arg_keys[1], (D,), jnp.float32), 0.1, 1.9)
    query_weight = gaussian(arg_keys[2], (D, HEADS * HD), D ** -0.5, 0.09375, ((0, 4), (1, 8)))
    key_weight = gaussian(arg_keys[3], (D, KV_HEADS * HD), D ** -0.5, 0.09375, ((0, 4), (1, 8)))
    value_weight = gaussian(arg_keys[4], (D, KV_HEADS * HD), D ** -0.5, 0.09375, ((0, 4), (1, 8)))
    query_gain = jnp.clip(1.0 + 0.18 * jax.random.normal(arg_keys[5], (HD,), jnp.float32), 0.1, 1.9)
    key_gain = jnp.clip(1.0 + 0.18 * jax.random.normal(arg_keys[6], (HD,), jnp.float32), 0.1, 1.9)
    head_offset = jnp.clip(-7.0 + 5.0 * jax.random.uniform(arg_keys[7], (HEADS,), jnp.float32) ** level_of(arg_keys[7], (HEADS,), ((0, 8),), -0.2, 0.2), -7.0, -2.0)
    key_cache = gaussian(arg_keys[8], (SEQS, CACHE, KV_HEADS * HD), 1.0, 6.0, ((0, 4), (2, 8)))
    value_cache = gaussian(arg_keys[9], (SEQS, CACHE, KV_HEADS * HD), 1.0, 6.0, ((0, 4), (2, 8)))
    lengths = set_ends(jax.random.randint(arg_keys[10], (SEQS,), 1, CACHE + 1), jax.random.fold_in(arg_keys[10], 1), 1, CACHE).astype(jnp.int32)
    out_weight = gaussian(arg_keys[11], (HEADS * HD, D), (HEADS * HD // 16) ** -0.5, 0.375, ((0, 8), (1, 4)))
    expert_gain = jnp.clip(1.0 + 0.18 * jax.random.normal(arg_keys[12], (D,), jnp.float32), 0.1, 1.9)
    routes_keys = jax.random.split(jax.random.fold_in(arg_keys[13], 1), SEQS // SEQ_DEV)
    routes_turns = jax.random.permutation(jax.random.fold_in(arg_keys[13], 3), SEQS // SEQ_DEV)
    routes = jax.vmap(lambda own, number: routed_block(jax.random.fold_in(arg_keys[13], 2), own, number, SEQ_DEV, EXPERTS, TOPK, CAP, 1))(routes_keys, routes_turns).reshape((SEQS, TOPK))
    route_weights = jnp.clip(0.1 + 0.9 * jax.random.uniform(arg_keys[14], (SEQS, TOPK), jnp.float32) ** level_of(arg_keys[14], (SEQS, TOPK), ((0, 4),), -0.2, 0.2), 0.1, 1.0)
    gate_weight = gaussian(arg_keys[15], (EXPERTS, D, D_EXP), D ** -0.5, 0.09375, ((0, 4), (2, 8)))
    up_weight = gaussian(arg_keys[16], (EXPERTS, D, D_EXP), D ** -0.5, 0.09375, ((0, 4), (2, 8)))
    down_weight = gaussian(arg_keys[17], (EXPERTS, D_EXP, D), D_EXP ** -0.5, 0.125, ((0, 4), (1, 8)))
    return {"hidden_in": hidden_in, "attn_gain": attn_gain, "query_weight": query_weight, "key_weight": key_weight, "value_weight": value_weight, "query_gain": query_gain, "key_gain": key_gain, "head_offset": head_offset, "key_cache": key_cache, "value_cache": value_cache, "lengths": lengths, "out_weight": out_weight, "expert_gain": expert_gain, "routes": routes, "route_weights": route_weights, "gate_weight": gate_weight, "up_weight": up_weight, "down_weight": down_weight}


EPSILON = 1e-06

def norm_rows(values, gain):
    meansq = lax.optimization_barrier(jnp.mean(values * values, axis=-1, keepdims=True))
    return values * lax.rsqrt(meansq + EPSILON) * gain

def reference(hidden_in, attn_gain, query_weight, key_weight, value_weight, query_gain, key_gain, head_offset, key_cache, value_cache, lengths, out_weight, expert_gain, routes, route_weights, gate_weight, up_weight, down_weight):
    groups = HEADS // KV_HEADS
    x_float = hidden_in.astype(jnp.float32)
    normed = norm_rows(x_float, attn_gain).astype(jnp.bfloat16)
    query_raw = jnp.dot(normed, query_weight, preferred_element_type=jnp.float32).astype(jnp.bfloat16)
    key_raw = jnp.dot(normed, key_weight, preferred_element_type=jnp.float32).astype(jnp.bfloat16)
    fresh_values = jnp.dot(normed, value_weight, preferred_element_type=jnp.float32).astype(jnp.bfloat16)
    query = norm_rows(query_raw.astype(jnp.float32).reshape(SEQS, HEADS, HD), query_gain).astype(jnp.bfloat16)
    fresh_keys = norm_rows(key_raw.astype(jnp.float32).reshape(SEQS, KV_HEADS, HD), key_gain).astype(jnp.bfloat16)
    offsets = head_offset.reshape(KV_HEADS, groups)

    def attend(args):
        query_row, key_rows, value_rows, length = args
        keys = key_rows.reshape(CACHE, KV_HEADS, HD).astype(jnp.float32)
        values = value_rows.reshape(CACHE, KV_HEADS, HD).astype(jnp.float32)
        grouped = query_row.reshape(KV_HEADS, groups, HD).astype(jnp.float32)
        scores = jnp.einsum('kgd,skd->kgs', grouped, keys) * HD ** (-0.5) + offsets[:, :, None]
        live = jnp.arange(CACHE, dtype=jnp.int32)[None, None, :] < length
        breaks = jnp.where(live, jax.nn.softplus(scores), 0.0)
        suffix = lax.cumsum(breaks, axis=2, reverse=True) - breaks
        stick = jnp.where(live, jnp.exp(jax.nn.log_sigmoid(scores) - suffix), 0.0).astype(jnp.bfloat16)
        result = jnp.einsum('kgs,skd->kgd', stick.astype(jnp.float32), values)
        return result.astype(jnp.bfloat16).reshape(HEADS * HD)
    attended = lax.map(attend, (query, key_cache, value_cache, lengths))
    projected = jnp.dot(attended, out_weight, preferred_element_type=jnp.float32)
    residual = (x_float + projected).astype(jnp.bfloat16)
    expert_in = norm_rows(residual.astype(jnp.float32), expert_gain).astype(jnp.bfloat16)

    def add_expert(total, index):
        gate = jnp.dot(expert_in, gate_weight[index], preferred_element_type=jnp.float32)
        upward = jnp.dot(expert_in, up_weight[index], preferred_element_type=jnp.float32)
        hidden = (jax.nn.silu(gate) * upward).astype(jnp.bfloat16)
        output = jnp.dot(hidden, down_weight[index], preferred_element_type=jnp.float32).astype(jnp.bfloat16)
        weight = lax.optimization_barrier(jnp.sum(jnp.where(routes == index, route_weights, 0.0), axis=1))
        return (total + weight[:, None] * output.astype(jnp.float32), None)
    mixed, _ = lax.scan(add_expert, jnp.zeros((SEQS, D), jnp.float32), jnp.arange(EXPERTS, dtype=jnp.int32))
    layer_out = (residual.astype(jnp.float32) + mixed).astype(jnp.bfloat16)
    return (layer_out, fresh_keys.reshape(SEQS, KV_HEADS * HD), fresh_values)
```

```python
import functools

import jax
import jax.numpy as jnp
from jax import lax
from jax.experimental import pallas as pl
from jax.experimental.pallas import tpu as pltpu
from jax.sharding import PartitionSpec as P

EPSILON = 1e-06
MESH = pl.DeviceIdType.MESH
F32 = jnp.float32
BF16 = jnp.bfloat16


def dot(a, b):
    return jnp.dot(a, b, preferred_element_type=F32)


def kernel(
    n_ep,
    n_tp,
    hid,
    attn_gain,
    wq_h,
    wk_h,
    wv_h,
    query_gain,
    key_gain,
    offset_s,
    kc_h,
    vc_h,
    lengths_s,
    wo_h,
    expert_gain,
    routes,
    route_weights,
    wg_h,
    wu_h,
    wd_h,
    out,
    fresh_k,
    fresh_v,
    hid_v,
    wq,
    wk,
    wv,
    kc,
    vc,
    wo,
    wg,
    wu,
    wd,
    xs,
    xf,
    part_s,
    part_r,
    q_s,
    z_s,
    st_s,
    o_s,
    att,
    p_s,
    p_r,
    res,
    y_s,
    y_r,
    m_s,
    m_r,
    local_sem,
    xs_sem,
    part_sem,
    att_sem,
    p_sem,
    res_sem,
    ep_sem,
    y_sem,
    m_sem,
):
    e = lax.axis_index("ep")
    t = lax.axis_index("tp")
    seqs, width = hid.shape
    feats = xs.shape[2]
    hd = query_gain.shape[1]
    qc = wq.shape[1]
    pc = wk.shape[1]
    heads = qc // hd
    kv = pc // hd
    groups = heads // kv
    cache = kc.shape[1]
    tokens = seqs * n_ep
    rows = tokens // n_tp
    per = seqs // rows
    share = width // n_tp

    def up_ep(j):
        return lax.rem(e + j, n_ep)

    def down_ep(j):
        return lax.rem(e + n_ep - j, n_ep)

    def up_tp(j):
        return lax.rem(t + j, n_tp)

    def down_tp(j):
        return lax.rem(t + n_tp - j, n_tp)

    def send(src, dst, sems, j, device):
        copy = pltpu.make_async_remote_copy(
            src_ref=src,
            dst_ref=dst,
            send_sem=sems.at[0, j],
            recv_sem=sems.at[1, j],
            device_id=device,
            device_id_type=MESH,
        )
        copy.start()
        return copy

    pairs = [
        (hid, hid_v),
        (hid.at[:, pl.ds(pl.multiple_of(e * feats, feats), feats)], xs.at[0]),
        (wq_h, wq),
        (wk_h, wk),
        (wv_h, wv),
        (kc_h, kc),
        (vc_h, vc),
        (wo_h, wo),
        (wg_h, wg),
        (wu_h, wu),
        (wd_h, wd),
    ]
    copies = [pltpu.make_async_copy(a, b, local_sem.at[i]) for i, (a, b) in enumerate(pairs)]
    for copy in copies:
        copy.start()
    c_hid, c_x0, c_q, c_k, c_v, c_kc, c_vc, c_wo, c_wg, c_wu, c_wd = copies

    barrier = pltpu.get_barrier_semaphore()
    for j in range(1, n_ep):
        pl.semaphore_signal(barrier, inc=1, device_id=(up_ep(j), t), device_id_type=MESH)
    for j in range(1, n_tp):
        pl.semaphore_signal(barrier, inc=1, device_id=(e, up_tp(j)), device_id_type=MESH)
    pl.semaphore_wait(barrier, n_ep + n_tp - 2)

    sent = []
    for j in range(1, n_ep):
        peer = up_ep(j)
        cols = pl.ds(pl.multiple_of(peer * feats, feats), feats)
        sent.append(send(hid.at[:, cols], xs.at[j], xs_sem, j - 1, (peer, t)))
    c_hid.wait()
    x = hid_v[...].astype(F32)
    scale = lax.rsqrt(jnp.mean(x * x, axis=1, keepdims=True) + EPSILON)
    c_x0.wait()
    gain = attn_gain[:, pl.ds(pl.multiple_of(e * feats, feats), feats)]
    for j in range(n_ep):
        if j > 0:
            sent[j - 1].wait()
        xj = xs[j].astype(F32)
        xf[j] = xj.reshape(per, rows, feats)
    lhs = jnp.concatenate([(xs[j].astype(F32) * gain).astype(BF16) for j in range(n_ep)], axis=0)
    c_q.wait()
    c_k.wait()
    c_v.wait()
    sums = jnp.concatenate([dot(lhs, wq[...]), dot(lhs, wk[...]), dot(lhs, wv[...])], axis=1)
    for j in range(n_ep):
        part_s[j] = sums[j * seqs : (j + 1) * seqs]
    sent = [send(part_s.at[j], part_r.at[j], part_sem, j - 1, (down_ep(j), t)) for j in range(1, n_ep)]
    total = part_s[0]
    for j in range(1, n_ep):
        sent[j - 1].wait()
        total = total + part_r[j]
    total = total * scale
    raw = total.astype(BF16)
    fresh_v[...] = raw[:, qc + pc :]
    rawf = raw.astype(F32)

    def head_norm(vals, g):
        return vals * lax.rsqrt(jnp.mean(vals * vals, axis=1, keepdims=True) + EPSILON) * g

    for k in range(kv):
        cols = slice(qc + k * hd, qc + (k + 1) * hd)
        fresh_k[:, k * hd : (k + 1) * hd] = head_norm(rawf[:, cols], key_gain[...]).astype(BF16)
    q_s[...] = jnp.zeros_like(q_s)
    for h in range(heads):
        q_s[h // groups, :, h % groups, :] = head_norm(rawf[:, h * hd : (h + 1) * hd], query_gain[...])

    lines = q_s.shape[2]
    span = min(256, cache)
    later = (
        lax.broadcasted_iota(jnp.int32, (span, span), 0)
        > lax.broadcasted_iota(jnp.int32, (span, span), 1)
    ).astype(BF16)
    place = lax.broadcasted_iota(jnp.int32, (1, lines, cache), 2)
    line = lax.broadcasted_iota(jnp.int32, (1, lines, 1), 1)
    inv = hd ** (-0.5)
    c_kc.wait()
    for k in range(kv):
        shift = jnp.zeros((1, lines, 1), F32)
        for g in range(groups):
            shift = jnp.where(line == g, offset_s[k * groups + g], shift)

        def score(b, carry, k=k, shift=shift):
            qb = q_s[k, b].astype(BF16)
            z = lax.dot_general(
                qb,
                kc[b, :, k * hd : (k + 1) * hd],
                (((1,), (1,)), ((), ())),
                preferred_element_type=F32,
            )
            z_s[pl.ds(b, 1)] = (z * inv)[None] + shift
            return carry

        lax.fori_loop(0, seqs, score, 0, unroll=True)

        limit = jnp.concatenate(
            [jnp.full((1, lines, 1), lengths_s[b], jnp.int32) for b in range(seqs)], axis=0
        )
        carry = jnp.zeros((seqs * lines, 1), F32)
        for c in reversed(range(cache // span)):
            z = z_s[:, :, c * span : (c + 1) * span]
            live = place[:, :, c * span : (c + 1) * span] < limit
            soft = jnp.log1p(jnp.exp(-jnp.abs(z)))
            breaks = jnp.where(live, jnp.maximum(z, 0.0) + soft, 0.0).reshape(seqs * lines, span)
            logsig = jnp.minimum(z, 0.0) - soft
            high = breaks.astype(BF16)
            mid = (breaks - high.astype(F32)).astype(BF16)
            suffix = dot(high, later) + dot(mid, later)
            after = (suffix + carry).reshape(seqs, lines, span)
            stick = jnp.where(live, jnp.exp(logsig - after), 0.0)
            st_s[:, :, c * span : (c + 1) * span] = stick
            carry = carry + suffix[:, 0:1] + breaks[:, 0:1]
        if k == 0:
            c_vc.wait()

        def mix(b, carry, k=k):
            o_s[k, pl.ds(b, 1)] = dot(st_s[b].astype(BF16), vc[b, :, k * hd : (k + 1) * hd])[None]
            return carry

        lax.fori_loop(0, seqs, mix, 0, unroll=True)
    for h in range(heads):
        att[0, :, h * hd : (h + 1) * hd] = o_s[h // groups, :, h % groups, :].astype(BF16)

    sent = [send(att.at[0], att.at[j], att_sem, j - 1, (up_ep(j), t)) for j in range(1, n_ep)]
    c_wo.wait()
    for j in range(n_ep):
        if j > 0:
            sent[j - 1].wait()
        block = dot(att[j], wo[...]).reshape(per, rows, feats).astype(BF16)
        p_s[pl.ds(down_ep(j) * per, per)] = block
    sent = [send(p_s.at[up_tp(j)], p_r.at[j], p_sem, j - 1, (e, up_tp(j))) for j in range(1, n_tp)]
    total = p_s[t].astype(F32)
    for j in range(1, n_tp):
        sent[j - 1].wait()
        total = total + p_r[j].astype(F32)
    owner = t // per
    slot = lax.rem(e + n_ep - owner, n_ep)
    res[0, t] = (xf[slot, lax.rem(t, per)] + total).astype(BF16)
    sent = [send(res.at[0, t], res.at[0, t], res_sem, j - 1, (e, up_tp(j))) for j in range(1, n_tp)]
    for copy in sent:
        copy.wait()
    sent = [send(res.at[0], res.at[j], ep_sem, j - 1, (up_ep(j), t)) for j in range(1, n_ep)]

    c_wg.wait()
    c_wu.wait()
    square = jnp.zeros((tokens, 1), F32)
    gate = jnp.zeros((tokens, wg.shape[2]), F32)
    upward = jnp.zeros((tokens, wg.shape[2]), F32)
    for j in range(n_ep):
        if j > 0:
            sent[j - 1].wait()
        at = pl.ds(pl.multiple_of(down_ep(j) * feats, feats), feats)
        r = res[j].astype(F32).reshape(tokens, feats)
        square = square + jnp.sum(r * r, axis=1, keepdims=True)
        r = (r * expert_gain[:, at]).astype(BF16)
        gate = gate + dot(r, wg[0, at, :])
        upward = upward + dot(r, wu[0, at, :])
    scale = lax.rsqrt(square / width + EPSILON)
    gate = gate * scale
    hidden = (gate * jax.nn.sigmoid(gate) * (upward * scale)).astype(BF16)
    c_wd.wait()
    for c in range(n_tp):
        block = dot(hidden, wd[0, :, c * share : (c + 1) * share]).astype(BF16)
        y_s[:, :, c * share : (c + 1) * share] = block.reshape(n_ep, seqs, share)

    sent = [send(y_s.at[up_ep(j)], y_r.at[j], y_sem, j - 1, (up_ep(j), t)) for j in range(1, n_ep)]
    mixed = jnp.zeros((seqs, width), F32)
    for j in range(n_ep):
        expert = down_ep(j)
        weight = jnp.sum(
            jnp.where(routes[...] == expert, route_weights[...], 0.0), axis=1, keepdims=True
        )
        if j > 0:
            sent[j - 1].wait()
            terms = y_r[j]
        else:
            terms = y_s[e]
        mixed = mixed + weight * terms.astype(F32)
    for c in range(n_tp):
        m_s[c] = mixed[:, c * share : (c + 1) * share].astype(BF16)
    sent = [send(m_s.at[up_tp(j)], m_r.at[j], m_sem, j - 1, (e, up_tp(j))) for j in range(1, n_tp)]
    holder = t * share // feats
    slot = lax.rem(e + n_ep - holder, n_ep)
    start = pl.multiple_of(lax.rem(t * share, feats), share)
    total = res[slot, pl.ds(e * per, per), :, pl.ds(start, share)].astype(F32).reshape(seqs, share)
    total = total + m_s[t].astype(F32)
    for j in range(1, n_tp):
        sent[j - 1].wait()
        total = total + m_r[j].astype(F32)
    out[...] = total.astype(BF16)


def body(
    hidden_in,
    attn_gain,
    query_weight,
    key_weight,
    value_weight,
    query_gain,
    key_gain,
    head_offset,
    key_cache,
    value_cache,
    lengths,
    out_weight,
    expert_gain,
    routes,
    route_weights,
    gate_weight,
    up_weight,
    down_weight,
):
    n_ep = lax.axis_size("ep")
    n_tp = lax.axis_size("tp")
    seqs, width = hidden_in.shape
    hd = query_gain.shape[0]
    feats, qc = query_weight.shape
    pc = key_weight.shape[1]
    kv = pc // hd
    lines = -(-(qc // pc) // 8) * 8
    cache = key_cache.shape[1]
    cols = out_weight.shape[1]
    tokens = seqs * n_ep
    rows = tokens // n_tp
    share = width // n_tp
    any_, vmem, smem = (
        pl.BlockSpec(memory_space=pl.ANY),
        pl.BlockSpec(memory_space=pltpu.VMEM),
        pl.BlockSpec(memory_space=pltpu.SMEM),
    )
    dma = pltpu.SemaphoreType.DMA

    def like(a):
        return pltpu.VMEM(a.shape, a.dtype)

    return pl.pallas_call(
        functools.partial(kernel, n_ep, n_tp),
        out_shape=(
            jax.ShapeDtypeStruct((seqs, share), BF16),
            jax.ShapeDtypeStruct((seqs, pc), BF16),
            jax.ShapeDtypeStruct((seqs, pc), BF16),
        ),
        in_specs=[
            any_, vmem, any_, any_, any_, vmem, vmem, smem, any_, any_, smem, any_, vmem, vmem,
            vmem, any_, any_, any_,
        ],
        out_specs=(vmem, vmem, vmem),
        scratch_shapes=[
            like(hidden_in),
            like(query_weight),
            like(key_weight),
            like(value_weight),
            like(key_cache),
            like(value_cache),
            like(out_weight),
            like(gate_weight),
            like(up_weight),
            like(down_weight),
            pltpu.VMEM((n_ep, seqs, feats), BF16),
            pltpu.VMEM((n_ep, seqs // rows, rows, feats), F32),
            pltpu.VMEM((n_ep, seqs, qc + 2 * pc), F32),
            pltpu.VMEM((n_ep, seqs, qc + 2 * pc), F32),
            pltpu.VMEM((kv, seqs, lines, hd), F32),
            pltpu.VMEM((seqs, lines, cache), F32),
            pltpu.VMEM((seqs, lines, cache), F32),
            pltpu.VMEM((kv, seqs, lines, hd), F32),
            pltpu.VMEM((n_ep, seqs, qc), BF16),
            pltpu.VMEM((n_tp, rows, cols), BF16),
            pltpu.VMEM((n_tp, rows, cols), BF16),
            pltpu.VMEM((n_ep, n_tp, rows, cols), BF16),
            pltpu.VMEM((n_ep, seqs, width), BF16),
            pltpu.VMEM((n_ep, seqs, width), BF16),
            pltpu.VMEM((n_tp, seqs, share), BF16),
            pltpu.VMEM((n_tp, seqs, share), BF16),
            dma((11,)),
            dma((2, n_ep - 1)),
            dma((2, n_ep - 1)),
            dma((2, n_ep - 1)),
            dma((2, n_tp - 1)),
            dma((2, n_tp - 1)),
            dma((2, n_ep - 1)),
            dma((2, n_ep - 1)),
            dma((2, n_tp - 1)),
        ],
        compiler_params=pltpu.CompilerParams(
            collective_id=0, has_side_effects=True, vmem_limit_bytes=60 * 2**20
        ),
    )(
        hidden_in,
        attn_gain.reshape(1, -1),
        query_weight,
        key_weight,
        value_weight,
        query_gain.reshape(1, -1),
        key_gain.reshape(1, -1),
        head_offset,
        key_cache,
        value_cache,
        lengths,
        out_weight,
        expert_gain.reshape(1, -1),
        routes,
        route_weights,
        gate_weight,
        up_weight,
        down_weight,
    )


def solution(mesh):
    placed = (
        P("ep", None),
        P(),
        P("ep", "tp"),
        P("ep", "tp"),
        P("ep", "tp"),
        P(),
        P(),
        P("tp"),
        P("ep", None, "tp"),
        P("ep", None, "tp"),
        P("ep"),
        P("tp", "ep"),
        P(),
        P("ep", None),
        P("ep", None),
        P("ep", None, "tp"),
        P("ep", None, "tp"),
        P("ep", "tp", None),
    )
    return jax.shard_map(
        body,
        mesh=mesh,
        in_specs=placed,
        out_specs=(P("ep", "tp"), P("ep", "tp"), P("ep", "tp")),
        check_vma=False,
    )
```

```python
import functools

import jax
import jax.numpy as jnp
from jax import lax
from jax.experimental import pallas as pl
from jax.experimental.pallas import tpu as pltpu
from jax.sharding import PartitionSpec as P

EPSILON = 1e-06
MESH = pl.DeviceIdType.MESH
F32 = jnp.float32
BF16 = jnp.bfloat16


def dot(a, b):
    return jnp.dot(a, b, preferred_element_type=F32)


def kernel(
    n_ep,
    n_tp,
    hid,
    attn_gain,
    wq_h,
    wk_h,
    wv_h,
    query_gain,
    key_gain,
    offset_s,
    kc_h,
    vc_h,
    lengths_s,
    wo_h,
    expert_gain,
    routes,
    route_weights,
    wg_h,
    wu_h,
    wd_h,
    out,
    fresh_k,
    fresh_v,
    hid_v,
    wq,
    wk,
    wv,
    kc,
    vc,
    wo,
    wg,
    wu,
    wd,
    xs,
    xf,
    part_s,
    part_r,
    q_s,
    z_s,
    st_s,
    o_s,
    att,
    p_s,
    p_r,
    res,
    d_s,
    d_r,
    y_s,
    y_r,
    m_s,
    m_r,
    local_sem,
    xs_sem,
    part_sem,
    att_sem,
    p_sem,
    res_sem,
    ep_sem,
    pair_sem,
    d_sem,
    y_sem,
    m_sem,
):
    e = lax.axis_index("ep")
    t = lax.axis_index("tp")
    seqs, width = hid.shape
    feats = xs.shape[2]
    hd = query_gain.shape[1]
    qc = wq.shape[1]
    pc = wk.shape[1]
    heads = qc // hd
    kv = pc // hd
    groups = heads // kv
    cache = kc.shape[1]
    tokens = seqs * n_ep
    rows = tokens // n_tp
    per = seqs // rows
    share = width // n_tp

    def up_ep(j):
        return lax.rem(e + j, n_ep)

    def down_ep(j):
        return lax.rem(e + n_ep - j, n_ep)

    def up_tp(j):
        return lax.rem(t + j, n_tp)

    def down_tp(j):
        return lax.rem(t + n_tp - j, n_tp)

    def send(src, dst, sems, j, device):
        copy = pltpu.make_async_remote_copy(
            src_ref=src,
            dst_ref=dst,
            send_sem=sems.at[0, j],
            recv_sem=sems.at[1, j],
            device_id=device,
            device_id_type=MESH,
        )
        copy.start()
        return copy

    pairs = [
        (hid, hid_v),
        (hid.at[:, pl.ds(pl.multiple_of(e * feats, feats), feats)], xs.at[0]),
        (wq_h, wq),
        (wk_h, wk),
        (wv_h, wv),
        (kc_h, kc),
        (vc_h, vc),
        (wo_h, wo),
        (wg_h, wg),
        (wu_h, wu),
        (wd_h, wd),
    ]
    copies = [pltpu.make_async_copy(a, b, local_sem.at[i]) for i, (a, b) in enumerate(pairs)]
    for copy in copies:
        copy.start()
    c_hid, c_x0, c_q, c_k, c_v, c_kc, c_vc, c_wo, c_wg, c_wu, c_wd = copies

    barrier = pltpu.get_barrier_semaphore()
    for j in range(1, n_ep):
        pl.semaphore_signal(barrier, inc=1, device_id=(up_ep(j), t), device_id_type=MESH)
    for j in range(1, n_tp):
        pl.semaphore_signal(barrier, inc=1, device_id=(e, up_tp(j)), device_id_type=MESH)
    weights = []
    same = lax.broadcasted_iota(jnp.int32, (seqs, seqs), 0) == lax.broadcasted_iota(
        jnp.int32, (seqs, seqs), 1
    )
    for j in range(n_ep):
        flat = jnp.sum(
            jnp.where(routes[...] == down_ep(j), route_weights[...], 0.0), axis=0, keepdims=True
        )
        weights.append(jnp.sum(jnp.where(same, flat, 0.0), axis=1, keepdims=True))
    c_hid.wait()
    pl.semaphore_wait(barrier, n_ep + n_tp - 2)

    sent = []
    for j in range(1, n_ep):
        peer = up_ep(j)
        cols = pl.ds(pl.multiple_of(peer * feats, feats), feats)
        sent.append(send(hid_v.at[:, cols], xs.at[j], xs_sem, j - 1, (peer, t)))
    x = hid_v[...].astype(F32)
    scale = lax.rsqrt(jnp.mean(x * x, axis=1, keepdims=True) + EPSILON)
    c_x0.wait()
    gain = attn_gain[:, pl.ds(pl.multiple_of(e * feats, feats), feats)]
    for j in range(n_ep):
        if j > 0:
            sent[j - 1].wait()
        xj = xs[j].astype(F32)
        xf[j] = xj.reshape(per, rows, feats)
    lhs = jnp.concatenate([(xs[j].astype(F32) * gain).astype(BF16) for j in range(n_ep)], axis=0)
    c_q.wait()
    c_k.wait()
    c_v.wait()
    sums = jnp.concatenate([dot(lhs, wq[...]), dot(lhs, wk[...]), dot(lhs, wv[...])], axis=1)
    for j in range(n_ep):
        part_s[j] = sums[j * seqs : (j + 1) * seqs].astype(BF16)
    sent = [send(part_s.at[j], part_r.at[j], part_sem, j - 1, (down_ep(j), t)) for j in range(1, n_ep)]
    total = sums[:seqs]
    for j in range(1, n_ep):
        sent[j - 1].wait()
        total = total + part_r[j].astype(F32)
    total = total * scale
    raw = total.astype(BF16)
    fresh_v[...] = raw[:, qc + pc :]
    rawf = raw.astype(F32)

    def head_norm(vals, g):
        return vals * lax.rsqrt(jnp.mean(vals * vals, axis=1, keepdims=True) + EPSILON) * g

    for k in range(kv):
        cols = slice(qc + k * hd, qc + (k + 1) * hd)
        fresh_k[:, k * hd : (k + 1) * hd] = head_norm(rawf[:, cols], key_gain[...]).astype(BF16)
    q_s[...] = jnp.zeros_like(q_s)
    for h in range(heads):
        q_s[h // groups, :, h % groups, :] = head_norm(rawf[:, h * hd : (h + 1) * hd], query_gain[...])

    lines = q_s.shape[2]
    span = min(256, cache)
    later = (
        lax.broadcasted_iota(jnp.int32, (span, span), 0)
        > lax.broadcasted_iota(jnp.int32, (span, span), 1)
    ).astype(BF16)
    place = lax.broadcasted_iota(jnp.int32, (1, lines, cache), 2)
    line = lax.broadcasted_iota(jnp.int32, (1, lines, 1), 1)
    inv = hd ** (-0.5)
    c_kc.wait()
    for k in range(kv):
        shift = jnp.zeros((1, lines, 1), F32)
        for g in range(groups):
            shift = jnp.where(line == g, offset_s[k * groups + g], shift)

        def score(b, carry, k=k, shift=shift):
            qb = q_s[k, b].astype(BF16)
            z = lax.dot_general(
                qb,
                kc[b, :, k * hd : (k + 1) * hd],
                (((1,), (1,)), ((), ())),
                preferred_element_type=F32,
            )
            z_s[pl.ds(b, 1)] = (z * inv)[None] + shift
            return carry

        lax.fori_loop(0, seqs, score, 0, unroll=True)

        limit = jnp.concatenate(
            [jnp.full((1, lines, 1), lengths_s[b], jnp.int32) for b in range(seqs)], axis=0
        )
        carry = jnp.zeros((seqs * lines, 1), F32)
        for c in reversed(range(cache // span)):
            z = z_s[:, :, c * span : (c + 1) * span]
            live = place[:, :, c * span : (c + 1) * span] < limit
            soft = jnp.log1p(jnp.exp(-jnp.abs(z)))
            breaks = jnp.where(live, jnp.maximum(z, 0.0) + soft, 0.0).reshape(seqs * lines, span)
            logsig = jnp.minimum(z, 0.0) - soft
            high = breaks.astype(BF16)
            mid = (breaks - high.astype(F32)).astype(BF16)
            suffix = dot(high, later) + dot(mid, later)
            after = (suffix + carry).reshape(seqs, lines, span)
            stick = jnp.where(live, jnp.exp(logsig - after), 0.0)
            st_s[:, :, c * span : (c + 1) * span] = stick
            carry = carry + suffix[:, 0:1] + breaks[:, 0:1]
        if k == 0:
            c_vc.wait()

        def mix(b, carry, k=k):
            o_s[k, pl.ds(b, 1)] = dot(st_s[b].astype(BF16), vc[b, :, k * hd : (k + 1) * hd])[None]
            return carry

        lax.fori_loop(0, seqs, mix, 0, unroll=True)
    for h in range(heads):
        att[0, :, h * hd : (h + 1) * hd] = o_s[h // groups, :, h % groups, :].astype(BF16)

    sent = [send(att.at[0], att.at[j], att_sem, j - 1, (up_ep(j), t)) for j in range(1, n_ep)]
    c_wo.wait()
    for j in range(n_ep):
        if j > 0:
            sent[j - 1].wait()
        block = dot(att[j], wo[...]).reshape(per, rows, feats).astype(BF16)
        p_s[pl.ds(down_ep(j) * per, per)] = block
    sent = [send(p_s.at[up_tp(j)], p_r.at[j], p_sem, j - 1, (e, up_tp(j))) for j in range(1, n_tp)]
    total = p_s[t].astype(F32)
    for j in range(1, n_tp):
        sent[j - 1].wait()
        total = total + p_r[j].astype(F32)
    owner = t // per
    slot = lax.rem(e + n_ep - owner, n_ep)
    res[0, t] = (xf[slot, lax.rem(t, per)] + total).astype(BF16)

    n_z = n_tp // 2
    z = t // 2
    core = lax.rem(t, 2)
    other = (e, z * 2 + 1 - core)

    def at_z(d):
        return lax.rem(z + d, n_z) * 2 + core

    def back_z(d):
        return lax.rem(z + n_z - d, n_z) * 2 + core

    along = [None] + [
        send(res.at[0, t], res.at[0, t], res_sem, d - 1, (e, at_z(d))) for d in range(1, n_z)
    ]
    across = {}
    paired = []
    for d in range(n_z):
        if d > 0:
            along[d].wait()
        piece = back_z(d)
        for j in range(1, n_ep):
            across[d, j] = send(
                res.at[0, piece],
                res.at[j, piece],
                ep_sem,
                d * (n_ep - 1) + j - 1,
                (up_ep(j), t),
            )
        paired.append(send(res.at[0, piece], res.at[0, piece], pair_sem, d, other))
    for d in range(n_z):
        piece = back_z(d)
        for j in range(1, n_ep):
            across[d, j].wait()
            at = d * (n_ep - 1) + j - 1 + n_z
            paired.append(send(res.at[j, piece], res.at[j, piece], pair_sem, at, other))

    c_wg.wait()
    c_wu.wait()
    square = jnp.zeros((tokens, 1), F32)
    gate = jnp.zeros((tokens, wg.shape[2]), F32)
    upward = jnp.zeros((tokens, wg.shape[2]), F32)
    for copy in paired:
        copy.wait()
    for j in range(n_ep):
        at = pl.ds(pl.multiple_of(down_ep(j) * feats, feats), feats)
        r = res[j].astype(F32).reshape(tokens, feats)
        square = square + jnp.sum(r * r, axis=1, keepdims=True)
        r = (r * expert_gain[:, at]).astype(BF16)
        gate = gate + dot(r, wg[0, at, :])
        upward = upward + dot(r, wu[0, at, :])
    scale = lax.rsqrt(square / width + EPSILON)
    gate = gate * scale
    hidden = (gate * jax.nn.sigmoid(gate) * (upward * scale)).astype(BF16)
    c_wd.wait()

    def down(block):
        at = pl.ds(pl.multiple_of(block * share, share), share)
        return dot(hidden, wd[0, :, at])

    turns = list(range(1, n_z)) + [0]
    paired = {}
    for d in turns:
        d_s[d] = down(lax.rem(z + d, n_z) * 2 + 1 - core).astype(BF16).reshape(n_ep, seqs, share)
        paired[d] = send(d_s.at[d], d_r.at[d], d_sem, d, other)
    across = {}
    for d in turns:
        mine = down(at_z(d)).reshape(n_ep, seqs, share)
        paired[d].wait()
        y_s[d] = (mine + d_r[d].astype(F32)).astype(BF16)
        for j in range(1, n_ep):
            across[d, j] = send(
                y_s.at[d, up_ep(j)],
                y_r.at[d, j],
                y_sem,
                d * (n_ep - 1) + j - 1,
                (up_ep(j), t),
            )
    along = []
    for d in turns:
        mixed = weights[0] * y_s[d, e].astype(F32)
        for j in range(1, n_ep):
            across[d, j].wait()
            mixed = mixed + weights[j] * y_r[d, j].astype(F32)
        if d > 0:
            m_s[d] = mixed.astype(BF16)
            along.append(send(m_s.at[d], m_r.at[d], m_sem, d - 1, (e, at_z(d))))
    holder = t * share // feats
    slot = lax.rem(e + n_ep - holder, n_ep)
    start = pl.multiple_of(lax.rem(t * share, feats), share)
    total = res[slot, pl.ds(e * per, per), :, pl.ds(start, share)].astype(F32).reshape(seqs, share)
    total = total + mixed
    for d in range(1, n_z):
        along[d - 1].wait()
        total = total + m_r[d].astype(F32)
    out[...] = total.astype(BF16)


def finish(a, b, c, a_out, b_out, c_out):
    a_out[...] = a[...]
    b_out[...] = b[...]
    c_out[...] = c[...]


def body(
    hidden_in,
    attn_gain,
    query_weight,
    key_weight,
    value_weight,
    query_gain,
    key_gain,
    head_offset,
    key_cache,
    value_cache,
    lengths,
    out_weight,
    expert_gain,
    routes,
    route_weights,
    gate_weight,
    up_weight,
    down_weight,
):
    n_ep = lax.axis_size("ep")
    n_tp = lax.axis_size("tp")
    seqs, width = hidden_in.shape
    hd = query_gain.shape[0]
    feats, qc = query_weight.shape
    pc = key_weight.shape[1]
    kv = pc // hd
    lines = -(-(qc // pc) // 8) * 8
    cache = key_cache.shape[1]
    cols = out_weight.shape[1]
    tokens = seqs * n_ep
    rows = tokens // n_tp
    share = width // n_tp
    n_z = n_tp // 2
    any_, vmem, smem = (
        pl.BlockSpec(memory_space=pl.ANY),
        pl.BlockSpec(memory_space=pltpu.VMEM),
        pl.BlockSpec(memory_space=pltpu.SMEM),
    )
    dma = pltpu.SemaphoreType.DMA

    def like(a):
        return pltpu.VMEM(a.shape, a.dtype)

    shapes = (
        jax.ShapeDtypeStruct((seqs, share), BF16),
        jax.ShapeDtypeStruct((seqs, pc), BF16),
        jax.ShapeDtypeStruct((seqs, pc), BF16),
    )
    results = pl.pallas_call(
        functools.partial(kernel, n_ep, n_tp),
        out_shape=shapes,
        in_specs=[
            any_, vmem, any_, any_, any_, vmem, vmem, smem, any_, any_, smem, any_, vmem, vmem,
            vmem, any_, any_, any_,
        ],
        out_specs=(vmem, vmem, vmem),
        scratch_shapes=[
            like(hidden_in),
            like(query_weight),
            like(key_weight),
            like(value_weight),
            like(key_cache),
            like(value_cache),
            like(out_weight),
            like(gate_weight),
            like(up_weight),
            like(down_weight),
            pltpu.VMEM((n_ep, seqs, feats), BF16),
            pltpu.VMEM((n_ep, seqs // rows, rows, feats), F32),
            pltpu.VMEM((n_ep, seqs, qc + 2 * pc), BF16),
            pltpu.VMEM((n_ep, seqs, qc + 2 * pc), BF16),
            pltpu.VMEM((kv, seqs, lines, hd), F32),
            pltpu.VMEM((seqs, lines, cache), F32),
            pltpu.VMEM((seqs, lines, cache), F32),
            pltpu.VMEM((kv, seqs, lines, hd), F32),
            pltpu.VMEM((n_ep, seqs, qc), BF16),
            pltpu.VMEM((n_tp, rows, cols), BF16),
            pltpu.VMEM((n_tp, rows, cols), BF16),
            pltpu.VMEM((n_ep, n_tp, rows, cols), BF16),
            pltpu.VMEM((n_z, n_ep, seqs, share), BF16),
            pltpu.VMEM((n_z, n_ep, seqs, share), BF16),
            pltpu.VMEM((n_z, n_ep, seqs, share), BF16),
            pltpu.VMEM((n_z, n_ep, seqs, share), BF16),
            pltpu.VMEM((n_z, seqs, share), BF16),
            pltpu.VMEM((n_z, seqs, share), BF16),
            dma((11,)),
            dma((2, n_ep - 1)),
            dma((2, n_ep - 1)),
            dma((2, n_ep - 1)),
            dma((2, n_tp - 1)),
            dma((2, n_z - 1)),
            dma((2, n_z * (n_ep - 1))),
            dma((2, n_z * n_ep)),
            dma((2, n_z)),
            dma((2, n_z * (n_ep - 1))),
            dma((2, n_z - 1)),
        ],
        compiler_params=pltpu.CompilerParams(
            collective_id=0, has_side_effects=True, vmem_limit_bytes=60 * 2**20
        ),
    )(
        hidden_in,
        attn_gain.reshape(1, -1),
        query_weight,
        key_weight,
        value_weight,
        query_gain.reshape(1, -1),
        key_gain.reshape(1, -1),
        head_offset,
        key_cache,
        value_cache,
        lengths,
        out_weight,
        expert_gain.reshape(1, -1),
        routes.T,
        route_weights.T,
        gate_weight,
        up_weight,
        down_weight,
    )
    return pl.pallas_call(
        finish,
        out_shape=shapes,
        in_specs=[vmem] * 3,
        out_specs=(vmem,) * 3,
    )(*results)


def solution(mesh):
    placed = (
        P("ep", None),
        P(),
        P("ep", "tp"),
        P("ep", "tp"),
        P("ep", "tp"),
        P(),
        P(),
        P("tp"),
        P("ep", None, "tp"),
        P("ep", None, "tp"),
        P("ep"),
        P("tp", "ep"),
        P(),
        P("ep", None),
        P("ep", None),
        P("ep", None, "tp"),
        P("ep", None, "tp"),
        P("ep", "tp", None),
    )
    return jax.shard_map(
        body,
        mesh=mesh,
        in_specs=placed,
        out_specs=(P("ep", "tp"), P("ep", "tp"), P("ep", "tp")),
        check_vma=False,
    )
```

```python
import functools

import jax
import jax.numpy as jnp
from jax import lax
from jax.experimental import pallas as pl
from jax.experimental.pallas import tpu as pltpu
from jax.sharding import PartitionSpec as P

EPSILON = 1e-06
MESH = pl.DeviceIdType.MESH
F32 = jnp.float32
BF16 = jnp.bfloat16


def dot(a, b):
    return jnp.dot(a, b, preferred_element_type=F32)


def kernel(
    n_ep,
    n_tp,
    hid,
    attn_gain_h,
    wq_h,
    wk_h,
    wv_h,
    query_gain_h,
    key_gain_h,
    offset_h,
    kc_h,
    vc_h,
    lengths_h,
    wo_h,
    expert_gain_h,
    routes_h,
    route_weights_h,
    wg_h,
    wu_h,
    wd_h,
    out,
    fresh_k,
    fresh_v,
    hid_v,
    attn_gain,
    query_gain,
    key_gain,
    offset,
    lengths,
    expert_gain,
    routes,
    route_weights,
    wq,
    wk,
    wv,
    kc,
    vc,
    wo,
    wg,
    wu,
    wd,
    xs,
    xf,
    part_s,
    part_r,
    q_s,
    z_s,
    st_s,
    o_s,
    att,
    p_s,
    p_r,
    res,
    d_s,
    d_r,
    y_s,
    y_r,
    m_s,
    m_r,
    local_sem,
    xs_sem,
    part_sem,
    att_sem,
    p_sem,
    res_sem,
    ep_sem,
    pair_sem,
    d_sem,
    y_sem,
    m_sem,
):
    e = lax.axis_index("ep")
    t = lax.axis_index("tp")
    seqs, width = hid.shape
    feats = xs.shape[2]
    hd = query_gain.shape[1]
    qc = wq.shape[1]
    pc = wk.shape[1]
    heads = qc // hd
    kv = pc // hd
    groups = heads // kv
    cache = kc.shape[1]
    tokens = seqs * n_ep
    rows = tokens // n_tp
    per = seqs // rows
    share = width // n_tp

    def up_ep(j):
        return lax.rem(e + j, n_ep)

    def down_ep(j):
        return lax.rem(e + n_ep - j, n_ep)

    def up_tp(j):
        return lax.rem(t + j, n_tp)

    def down_tp(j):
        return lax.rem(t + n_tp - j, n_tp)

    def send(src, dst, sems, j, device):
        copy = pltpu.make_async_remote_copy(
            src_ref=src,
            dst_ref=dst,
            send_sem=sems.at[0, j],
            recv_sem=sems.at[1, j],
            device_id=device,
            device_id_type=MESH,
        )
        copy.start()
        return copy

    barrier = pltpu.get_barrier_semaphore()
    for j in range(1, n_ep):
        pl.semaphore_signal(barrier, inc=1, device_id=(up_ep(j), t), device_id_type=MESH)
    for j in range(1, n_tp):
        pl.semaphore_signal(barrier, inc=1, device_id=(e, up_tp(j)), device_id_type=MESH)

    pairs = [
        (hid, hid_v),
        (attn_gain_h, attn_gain),
        (query_gain_h, query_gain),
        (key_gain_h, key_gain),
        (offset_h, offset),
        (lengths_h, lengths),
        (expert_gain_h, expert_gain),
        (routes_h, routes),
        (route_weights_h, route_weights),
        (hid.at[:, pl.ds(pl.multiple_of(e * feats, feats), feats)], xs.at[0]),
        (wq_h, wq),
        (wk_h, wk),
        (wv_h, wv),
        (kc_h, kc),
        (vc_h, vc),
        (wo_h, wo),
        (wg_h, wg),
        (wu_h, wu),
        (wd_h, wd),
    ]
    copies = [pltpu.make_async_copy(a, b, local_sem.at[i]) for i, (a, b) in enumerate(pairs)]
    for copy in copies:
        copy.start()
    c_hid, *c_small, c_x0, c_q, c_k, c_v, c_kc, c_vc, c_wo, c_wg, c_wu, c_wd = copies

    for copy in c_small:
        copy.wait()
    weights = []
    same = lax.broadcasted_iota(jnp.int32, (seqs, seqs), 0) == lax.broadcasted_iota(
        jnp.int32, (seqs, seqs), 1
    )
    for j in range(n_ep):
        flat = jnp.sum(
            jnp.where(routes[...] == down_ep(j), route_weights[...], 0.0), axis=0, keepdims=True
        )
        weights.append(jnp.sum(jnp.where(same, flat, 0.0), axis=1, keepdims=True))
    c_hid.wait()
    pl.semaphore_wait(barrier, n_ep + n_tp - 2)

    sent = []
    for j in range(1, n_ep):
        peer = up_ep(j)
        cols = pl.ds(pl.multiple_of(peer * feats, feats), feats)
        sent.append(send(hid_v.at[:, cols], xs.at[j], xs_sem, j - 1, (peer, t)))
    x = hid_v[...].astype(F32)
    scale = lax.rsqrt(jnp.mean(x * x, axis=1, keepdims=True) + EPSILON)
    c_x0.wait()
    gain = attn_gain[:, pl.ds(pl.multiple_of(e * feats, feats), feats)]
    for j in range(n_ep):
        if j > 0:
            sent[j - 1].wait()
        xj = xs[j].astype(F32)
        xf[j] = xj.reshape(per, rows, feats)
    lhs = jnp.concatenate([(xs[j].astype(F32) * gain).astype(BF16) for j in range(n_ep)], axis=0)
    c_q.wait()
    c_k.wait()
    c_v.wait()
    sums = jnp.concatenate([dot(lhs, wq[...]), dot(lhs, wk[...]), dot(lhs, wv[...])], axis=1)
    for j in range(n_ep):
        part_s[j] = sums[j * seqs : (j + 1) * seqs].astype(BF16)
    sent = [send(part_s.at[j], part_r.at[j], part_sem, j - 1, (down_ep(j), t)) for j in range(1, n_ep)]
    total = sums[:seqs]
    for j in range(1, n_ep):
        sent[j - 1].wait()
        total = total + part_r[j].astype(F32)
    total = total * scale
    raw = total.astype(BF16)
    fresh_v[...] = raw[:, qc + pc :]
    rawf = raw.astype(F32)

    def head_norm(vals, g):
        return vals * lax.rsqrt(jnp.mean(vals * vals, axis=1, keepdims=True) + EPSILON) * g

    for k in range(kv):
        cols = slice(qc + k * hd, qc + (k + 1) * hd)
        fresh_k[:, k * hd : (k + 1) * hd] = head_norm(rawf[:, cols], key_gain[...]).astype(BF16)
    q_s[...] = jnp.zeros_like(q_s)
    for h in range(heads):
        q_s[h // groups, :, h % groups, :] = head_norm(rawf[:, h * hd : (h + 1) * hd], query_gain[...])

    lines = q_s.shape[2]
    span = min(256, cache)
    later = (
        lax.broadcasted_iota(jnp.int32, (span, span), 0)
        > lax.broadcasted_iota(jnp.int32, (span, span), 1)
    ).astype(BF16)
    place = lax.broadcasted_iota(jnp.int32, (1, lines, cache), 2)
    line = lax.broadcasted_iota(jnp.int32, (1, lines, 1), 1)
    inv = hd ** (-0.5)
    c_kc.wait()
    for k in range(kv):
        shift = jnp.zeros((1, lines, 1), F32)
        for g in range(groups):
            shift = jnp.where(line == g, offset[:, k * groups + g : k * groups + g + 1][None], shift)

        def score(b, carry, k=k, shift=shift):
            qb = q_s[k, b].astype(BF16)
            z = lax.dot_general(
                qb,
                kc[b, :, k * hd : (k + 1) * hd],
                (((1,), (1,)), ((), ())),
                preferred_element_type=F32,
            )
            z_s[pl.ds(b, 1)] = (z * inv)[None] + shift
            return carry

        lax.fori_loop(0, seqs, score, 0, unroll=True)

        limit = jnp.concatenate(
            [jnp.broadcast_to(lengths[:, b : b + 1][None], (1, lines, 1)) for b in range(seqs)], axis=0
        )
        carry = jnp.zeros((seqs * lines, 1), F32)
        for c in reversed(range(cache // span)):
            z = z_s[:, :, c * span : (c + 1) * span]
            live = place[:, :, c * span : (c + 1) * span] < limit
            soft = jnp.log1p(jnp.exp(-jnp.abs(z)))
            breaks = jnp.where(live, jnp.maximum(z, 0.0) + soft, 0.0).reshape(seqs * lines, span)
            logsig = jnp.minimum(z, 0.0) - soft
            high = breaks.astype(BF16)
            mid = (breaks - high.astype(F32)).astype(BF16)
            suffix = dot(high, later) + dot(mid, later)
            after = (suffix + carry).reshape(seqs, lines, span)
            stick = jnp.where(live, jnp.exp(logsig - after), 0.0)
            st_s[:, :, c * span : (c + 1) * span] = stick
            carry = carry + suffix[:, 0:1] + breaks[:, 0:1]
        if k == 0:
            c_vc.wait()

        def mix(b, carry, k=k):
            o_s[k, pl.ds(b, 1)] = dot(st_s[b].astype(BF16), vc[b, :, k * hd : (k + 1) * hd])[None]
            return carry

        lax.fori_loop(0, seqs, mix, 0, unroll=True)
    for h in range(heads):
        att[0, :, h * hd : (h + 1) * hd] = o_s[h // groups, :, h % groups, :].astype(BF16)

    sent = [send(att.at[0], att.at[j], att_sem, j - 1, (up_ep(j), t)) for j in range(1, n_ep)]
    c_wo.wait()
    for j in range(n_ep):
        if j > 0:
            sent[j - 1].wait()
        block = dot(att[j], wo[...]).reshape(per, rows, feats).astype(BF16)
        p_s[pl.ds(down_ep(j) * per, per)] = block
    sent = [send(p_s.at[up_tp(j)], p_r.at[j], p_sem, j - 1, (e, up_tp(j))) for j in range(1, n_tp)]
    total = p_s[t].astype(F32)
    for j in range(1, n_tp):
        sent[j - 1].wait()
        total = total + p_r[j].astype(F32)
    owner = t // per
    slot = lax.rem(e + n_ep - owner, n_ep)
    res[0, t] = (xf[slot, lax.rem(t, per)] + total).astype(BF16)

    n_z = n_tp // 2
    z = t // 2
    core = lax.rem(t, 2)
    other = (e, z * 2 + 1 - core)

    def at_z(d):
        return lax.rem(z + d, n_z) * 2 + core

    def back_z(d):
        return lax.rem(z + n_z - d, n_z) * 2 + core

    along = [None] + [
        send(res.at[0, t], res.at[0, t], res_sem, d - 1, (e, at_z(d))) for d in range(1, n_z)
    ]
    across = {}
    paired = {}
    for d in range(n_z):
        if d > 0:
            along[d].wait()
        piece = back_z(d)
        for j in range(1, n_ep):
            across[d, j] = send(
                res.at[0, piece],
                res.at[j, piece],
                ep_sem,
                d * (n_ep - 1) + j - 1,
                (up_ep(j), t),
            )
        paired[d, 0] = send(res.at[0, piece], res.at[0, piece], pair_sem, d, other)
    def forward(j):
        for d in range(n_z):
            piece = back_z(d)
            across[d, j].wait()
            at = d * (n_ep - 1) + j - 1 + n_z
            paired[d, j] = send(res.at[j, piece], res.at[j, piece], pair_sem, at, other)

    c_wg.wait()
    c_wu.wait()
    square = jnp.zeros((tokens, 1), F32)
    gate = jnp.zeros((tokens, wg.shape[2]), F32)
    upward = jnp.zeros((tokens, wg.shape[2]), F32)
    for j in range(n_ep):
        if j + 1 < n_ep:
            forward(j + 1)
        for d in range(n_z):
            paired[d, j].wait()
        at = pl.ds(pl.multiple_of(down_ep(j) * feats, feats), feats)
        r = res[j].astype(F32).reshape(tokens, feats)
        square = square + jnp.sum(r * r, axis=1, keepdims=True)
        r = (r * expert_gain[:, at]).astype(BF16)
        gate = gate + dot(r, wg[0, at, :])
        upward = upward + dot(r, wu[0, at, :])
    scale = lax.rsqrt(square / width + EPSILON)
    gate = gate * scale
    hidden = (gate * jax.nn.sigmoid(gate) * (upward * scale)).astype(BF16)
    c_wd.wait()

    def down(block):
        at = pl.ds(pl.multiple_of(block * share, share), share)
        return dot(hidden, wd[0, :, at])

    turns = list(range(1, n_z)) + [0]
    paired = {}
    for d in turns:
        d_s[d] = down(lax.rem(z + d, n_z) * 2 + 1 - core).astype(BF16).reshape(n_ep, seqs, share)
        paired[d] = send(d_s.at[d], d_r.at[d], d_sem, d, other)
    across = {}
    for d in turns:
        mine = down(at_z(d)).reshape(n_ep, seqs, share)
        paired[d].wait()
        y_s[d] = (mine + d_r[d].astype(F32)).astype(BF16)
        for j in range(1, n_ep):
            across[d, j] = send(
                y_s.at[d, up_ep(j)],
                y_r.at[d, j],
                y_sem,
                d * (n_ep - 1) + j - 1,
                (up_ep(j), t),
            )
    along = []
    for d in turns:
        mixed = weights[0] * y_s[d, e].astype(F32)
        for j in range(1, n_ep):
            across[d, j].wait()
            mixed = mixed + weights[j] * y_r[d, j].astype(F32)
        if d > 0:
            m_s[d] = mixed.astype(BF16)
            along.append(send(m_s.at[d], m_r.at[d], m_sem, d - 1, (e, at_z(d))))
    holder = t * share // feats
    slot = lax.rem(e + n_ep - holder, n_ep)
    start = pl.multiple_of(lax.rem(t * share, feats), share)
    total = res[slot, pl.ds(e * per, per), :, pl.ds(start, share)].astype(F32).reshape(seqs, share)
    total = total + mixed
    for d in range(1, n_z):
        along[d - 1].wait()
        total = total + m_r[d].astype(F32)
    out[...] = total.astype(BF16)


def finish(a, b, c, a_out, b_out, c_out):
    a_out[...] = a[...]
    b_out[...] = b[...]
    c_out[...] = c[...]


def body(
    hidden_in,
    attn_gain,
    query_weight,
    key_weight,
    value_weight,
    query_gain,
    key_gain,
    head_offset,
    key_cache,
    value_cache,
    lengths,
    out_weight,
    expert_gain,
    routes,
    route_weights,
    gate_weight,
    up_weight,
    down_weight,
):
    n_ep = lax.axis_size("ep")
    n_tp = lax.axis_size("tp")
    seqs, width = hidden_in.shape
    hd = query_gain.shape[0]
    feats, qc = query_weight.shape
    pc = key_weight.shape[1]
    kv = pc // hd
    lines = -(-(qc // pc) // 8) * 8
    cache = key_cache.shape[1]
    cols = out_weight.shape[1]
    tokens = seqs * n_ep
    rows = tokens // n_tp
    share = width // n_tp
    n_z = n_tp // 2
    any_ = pl.BlockSpec(memory_space=pl.ANY)
    vmem = pl.BlockSpec(memory_space=pltpu.VMEM)
    dma = pltpu.SemaphoreType.DMA

    def like(a):
        return pltpu.VMEM(a.shape, a.dtype)

    shapes = (
        jax.ShapeDtypeStruct((seqs, share), BF16),
        jax.ShapeDtypeStruct((seqs, pc), BF16),
        jax.ShapeDtypeStruct((seqs, pc), BF16),
    )
    results = pl.pallas_call(
        functools.partial(kernel, n_ep, n_tp),
        out_shape=shapes,
        in_specs=[
            any_,
        ] * 18,
        out_specs=(vmem, vmem, vmem),
        scratch_shapes=[
            like(hidden_in),
            pltpu.VMEM((1, width), F32),
            pltpu.VMEM((1, hd), F32),
            pltpu.VMEM((1, hd), F32),
            pltpu.VMEM((1, head_offset.shape[0]), F32),
            pltpu.VMEM((1, seqs), jnp.int32),
            pltpu.VMEM((1, width), F32),
            pltpu.VMEM(routes.shape[::-1], jnp.int32),
            pltpu.VMEM(routes.shape[::-1], F32),
            like(query_weight),
            like(key_weight),
            like(value_weight),
            like(key_cache),
            like(value_cache),
            like(out_weight),
            like(gate_weight),
            like(up_weight),
            like(down_weight),
            pltpu.VMEM((n_ep, seqs, feats), BF16),
            pltpu.VMEM((n_ep, seqs // rows, rows, feats), F32),
            pltpu.VMEM((n_ep, seqs, qc + 2 * pc), BF16),
            pltpu.VMEM((n_ep, seqs, qc + 2 * pc), BF16),
            pltpu.VMEM((kv, seqs, lines, hd), F32),
            pltpu.VMEM((seqs, lines, cache), F32),
            pltpu.VMEM((seqs, lines, cache), F32),
            pltpu.VMEM((kv, seqs, lines, hd), F32),
            pltpu.VMEM((n_ep, seqs, qc), BF16),
            pltpu.VMEM((n_tp, rows, cols), BF16),
            pltpu.VMEM((n_tp, rows, cols), BF16),
            pltpu.VMEM((n_ep, n_tp, rows, cols), BF16),
            pltpu.VMEM((n_z, n_ep, seqs, share), BF16),
            pltpu.VMEM((n_z, n_ep, seqs, share), BF16),
            pltpu.VMEM((n_z, n_ep, seqs, share), BF16),
            pltpu.VMEM((n_z, n_ep, seqs, share), BF16),
            pltpu.VMEM((n_z, seqs, share), BF16),
            pltpu.VMEM((n_z, seqs, share), BF16),
            dma((19,)),
            dma((2, n_ep - 1)),
            dma((2, n_ep - 1)),
            dma((2, n_ep - 1)),
            dma((2, n_tp - 1)),
            dma((2, n_z - 1)),
            dma((2, n_z * (n_ep - 1))),
            dma((2, n_z * n_ep)),
            dma((2, n_z)),
            dma((2, n_z * (n_ep - 1))),
            dma((2, n_z - 1)),
        ],
        compiler_params=pltpu.CompilerParams(
            collective_id=0, has_side_effects=True, vmem_limit_bytes=60 * 2**20
        ),
    )(
        hidden_in,
        attn_gain.reshape(1, -1),
        query_weight,
        key_weight,
        value_weight,
        query_gain.reshape(1, -1),
        key_gain.reshape(1, -1),
        head_offset.reshape(1, -1),
        key_cache,
        value_cache,
        lengths.reshape(1, -1),
        out_weight,
        expert_gain.reshape(1, -1),
        routes.T,
        route_weights.T,
        gate_weight,
        up_weight,
        down_weight,
    )
    return pl.pallas_call(
        finish,
        out_shape=shapes,
        in_specs=[vmem] * 3,
        out_specs=(vmem,) * 3,
    )(*results)


def solution(mesh):
    placed = (
        P("ep", None),
        P(),
        P("ep", "tp"),
        P("ep", "tp"),
        P("ep", "tp"),
        P(),
        P(),
        P("tp"),
        P("ep", None, "tp"),
        P("ep", None, "tp"),
        P("ep"),
        P("tp", "ep"),
        P(),
        P("ep", None),
        P("ep", None),
        P("ep", None, "tp"),
        P("ep", None, "tp"),
        P("ep", "tp", None),
    )
    return jax.shard_map(
        body,
        mesh=mesh,
        in_specs=placed,
        out_specs=(P("ep", "tp"), P("ep", "tp"), P("ep", "tp")),
        check_vma=False,
    )
```
